256 devices in a mesh: sp: 64 (over z, y, core), tp: 4 (over x).
Axes of the slice: x: 4, y: 4, z: 8, core: 2. Of those that a mesh axis runs over, the one named last changes fastest.
Arguments:
- residual: bfloat16 [65536, 2048], P(('sp', 'tp')), may hold values from -6 to 6
- pool_input: bfloat16 [65536, 1024], P('sp', 'tp'), may hold values from -6 to 6
- doc_ids: int32 [65536], P('sp'), may hold values from 0 to 31, never falling along the last dimension, each value on 1 to 4096 neighbouring positions
- pool_map: bfloat16 [4, 256, 256], P('tp'), may hold values from -0.375 to 0.375
- pool_scale: float32 [1024], P('tp'), may hold values from 0.1 to 1.9
- out_weight: bfloat16 [1024, 2048], replicated, may hold values from -0.1875 to 0.1875
- mix_gain: float32 [2048], replicated, may hold values from 0.1 to 1.9
- mix_shift: float32 [2048], replicated, may hold values from -1.75 to 1.75
- group_router: bfloat16 [2048, 4], replicated, may hold values from -0.125 to 0.125
- expert_router: bfloat16 [2048, 64], replicated, may hold values from -0.125 to 0.125
- expert_gate: bfloat16 [64, 2048, 512], P('sp'), may hold values from -0.375 to 0.375
- expert_up: bfloat16 [64, 2048, 512], P('sp'), may hold values from -0.375 to 0.375
- expert_down: bfloat16 [64, 512, 2048], P('sp'), may hold values from -0.75 to 0.75
- routes: int32 [65536, 2], P(('sp', 'tp')), may hold values from 0 to 63, as said below
- ffn_gain: float32 [2048], replicated, may hold values from 0.1 to 1.9
- ffn_shift: float32 [2048], replicated, may hold values from -1.75 to 1.75
Outputs:
- layer_out: bfloat16 [65536, 2048], P(('sp', 'tp'))
The draws below stay inside these ranges and needn't reach their ends.
Inputs may be any that keep to these rules, and one draw needn't show every extreme that they name: `doc_ids`: document numbers never fall along the positions; each document has 1 to 4096 positions. `routes`: A token names 2 different experts. In each aligned block of half of one device's 256 rows, 32 experts are named exactly 8 times each and the others not at all.
All inputs are finite; a program needn't handle non-finite values.
Results may differ from the reference program's by a relative error of at most 0.0073.
Values may be sent and summed in bfloat16 or wider, within the bound.
No kernel may reach another device: no remote copies, remote signals or barrier semaphores. Data moves between devices by JAX's collectives and lax.ppermute only.
A program may use at most 128 MiB of HBM per device.

```python
import math
import jax
import jax.numpy as jnp
import numpy as np
from jax import lax

D = 2048
POOL = 1024
PGROUPS = 4
GW = 256
FF = 512
MGROUPS = 4
TOPK = 2
SEQ_DEV = 1024
ROWS = 256
TOKENS = 65536
EXPERTS = 64
SLOTS = 8
N_SP = 64


def draw_routes(key, part):
    block_rows = ROWS // 2
    block_count = TOKENS // block_rows
    named_count = EXPERTS // 2
    anchor = jax.random.randint(jax.random.fold_in(key, 7), (), 0, EXPERTS).astype(jnp.int32)
    block_seeds = jax.random.split(jax.random.fold_in(key, 11), block_count)

    def one_block(block_seed):
        seeds = jax.random.split(block_seed, TOPK + 2)
        others = (anchor + 1 + jax.random.permutation(seeds[0], EXPERTS - 1).astype(jnp.int32)) % EXPERTS
        chosen = jnp.concatenate([anchor[None], others[:named_count - 1]]).astype(jnp.int32)
        listed = chosen[jnp.arange(named_count * SLOTS, dtype=jnp.int32) // SLOTS]
        columns = []
        for column in range(TOPK):
            segment = listed[column * block_rows:(column + 1) * block_rows]
            order = jax.random.permutation(seeds[column + 1], block_rows).astype(jnp.int32)
            columns.append(segment[order])
        table = jnp.stack(columns, axis=1)
        rotation = jax.random.randint(seeds[TOPK + 1], (block_rows,), 0, TOPK).astype(jnp.int32)
        column_index = (jnp.arange(TOPK, dtype=jnp.int32)[None, :] + rotation[:, None]) % TOPK
        return jnp.take_along_axis(table, column_index, axis=1)
    blocks = jax.vmap(one_block)(block_seeds)
    return blocks.reshape(TOKENS, TOPK).astype(jnp.int32)


def level_of(stream_key, shape, shards, low, high):
    level, own = 1.0, jax.random.fold_in(stream_key, 6)
    for position, shards_of in shards:
        steps = jnp.exp(jax.random.uniform(jax.random.fold_in(own, position), (shards_of,), jnp.float32, low / len(shards), high / len(shards)))
        level = level * jnp.repeat(steps, shape[position] // shards_of).reshape([-1 if axis == position else 1 for axis in range(len(shape))])
    return level


def length_profile(amount, total, bound, lean):
    portions = [(1 << 20) // math.isqrt(rank ** lean) + 1 for rank in range(2, amount + 1)]
    spare, given = total - bound - (amount - 1), [1] * (amount - 1)
    while spare > 0:
        free = [i for i in range(amount - 1) if given[i] < bound]
        pool, remaining = sum([portions[i] for i in free]), spare
        for i in free:
            extra = min(bound - given[i], max(1, remaining * portions[i] // pool), spare)
            given[i] = given[i] + extra
            spare = spare - extra
    return np.array([bound] + given)


def uneven(stream_key, number_of, total, limit, slope):
    if number_of == 2:
        one = jax.random.randint(stream_key, (), max(1, total - limit), min(limit, total - 1) + 1)
        return jnp.stack([one, total - one])
    tallies = jnp.asarray(length_profile(number_of, total, limit, slope), jnp.int32)
    couples = (number_of - 1) // 2
    source_of, taker = tallies[1:1 + 2 * couples:2], tallies[2:2 + 2 * couples:2]
    slack = jnp.minimum(source_of - 1, limit - taker)
    moved = jax.random.randint(jax.random.fold_in(stream_key, 1), (couples,), 0, 1 << 20) % (slack + 1)
    tallies = tallies.at[1:1 + 2 * couples:2].set(source_of - moved).at[2:2 + 2 * couples:2].set(taker + moved)
    return tallies[jax.random.permutation(jax.random.fold_in(stream_key, 2), number_of)]


def bell_draw(rng, dims, width, reach, cuts=(), kind=jnp.bfloat16):
    values = jax.random.normal(rng, dims, jnp.float32) * width
    if len(cuts) > 0:
        values = level_of(rng, dims, cuts, -0.22, 0.18) * values
    return jnp.clip(values, min=-reach, max=reach).astype(kind)


def setup_inputs(seed: int = 0) -> dict:
    key_list = jax.random.split(jax.random.key(seed), 17)
    residual = bell_draw(key_list[0], (TOKENS, D), 1.0, 6.0, ((0, 256),))
    pool_input = bell_draw(key_list[1], (TOKENS, POOL), 1.0, 6.0, ((0, 64), (1, 4)))
    doc_ids = jnp.searchsorted(jnp.cumsum(uneven(key_list[2], N_SP // 2, TOKENS, 4 * SEQ_DEV, 1)), jnp.arange(TOKENS), side="right").astype(jnp.int32)
    pool_map = bell_draw(key_list[3], (PGROUPS, GW, GW), GW ** -0.5, 0.375, ((0, 4),))
    pool_scale = jnp.clip(1.0 + 0.18 * jax.random.normal(key_list[4], (POOL,), jnp.float32), 0.1, 1.9)
    out_weight = bell_draw(key_list[5], (POOL, D), POOL ** -0.5, 0.1875)
    mix_gain = jnp.clip(1.0 + 0.18 * jax.random.normal(key_list[6], (D,), jnp.float32), 0.1, 1.9)
    mix_shift = bell_draw(key_list[7], (D,), 0.3, 1.75, (), jnp.float32)
    group_router = bell_draw(key_list[8], (D, MGROUPS), D ** -0.5, 0.125)
    expert_router = bell_draw(key_list[9], (D, EXPERTS), D ** -0.5, 0.125)
    expert_gate = bell_draw(key_list[10], (EXPERTS, D, FF), (D // 8) ** -0.5, 0.375, ((0, 64),))
    expert_up = bell_draw(key_list[11], (EXPERTS, D, FF), (D // 8) ** -0.5, 0.375, ((0, 64),))
    expert_down = bell_draw(key_list[12], (EXPERTS, FF, D), (FF // 8) ** -0.5, 0.75, ((0, 64),))
    routes = draw_routes(jax.random.fold_in(key_list[16], 71), 0)
    ffn_gain = jnp.clip(1.0 + 0.18 * jax.random.normal(key_list[14], (D,), jnp.float32), 0.1, 1.9)
    ffn_shift = bell_draw(key_list[15], (D,), 0.3, 1.75, (), jnp.float32)
    return {"residual": residual, "pool_input": pool_input, "doc_ids": doc_ids, "pool_map": pool_map, "pool_scale": pool_scale, "out_weight": out_weight, "mix_gain": mix_gain, "mix_shift": mix_shift, "group_router": group_router, "expert_router": expert_router, "expert_gate": expert_gate, "expert_up": expert_up, "expert_down": expert_down, "routes": routes, "ffn_gain": ffn_gain, "ffn_shift": ffn_shift}


skip_scale = 2.0 ** 0.5
epsilon = 1e-05

def layer_norm(values, norm_gain, norm_shift):
    center = values - lax.optimization_barrier(jnp.mean(values, axis=-1, keepdims=True))
    spread = lax.optimization_barrier(jnp.mean(center * center, axis=-1, keepdims=True))
    return center * lax.rsqrt(spread + epsilon) * norm_gain + norm_shift

def route_weights(normed, chosen, group_router, expert_router):
    group_logits = jnp.dot(normed, group_router, preferred_element_type=jnp.float32)
    expert_logits = jnp.dot(normed, expert_router, preferred_element_type=jnp.float32)
    group_count = group_logits.shape[1]
    expert_count = expert_logits.shape[1]
    group_exp = jnp.exp(group_logits)
    group_prob = group_exp / lax.optimization_barrier(jnp.sum(group_exp, axis=1, keepdims=True))
    expert_ids = jnp.arange(expert_count, dtype=jnp.int32)
    picked = lax.optimization_barrier(jnp.sum(jnp.where(chosen[:, :, None] == expert_ids[None, None, :], expert_logits[:, None, :], 0.0), axis=2))
    picked_exp = jnp.exp(picked)
    pair_share = picked_exp / lax.optimization_barrier(jnp.sum(picked_exp, axis=1, keepdims=True))
    group_of = chosen // (expert_count // group_count)
    group_ids = jnp.arange(group_count, dtype=jnp.int32)
    group_share = lax.optimization_barrier(jnp.sum(jnp.where(group_of[:, :, None] == group_ids[None, None, :], group_prob[:, None, :], 0.0), axis=2))
    return group_share * pair_share

def pool_group(values, doc_ids, window):
    length = values.shape[0]
    source = values.astype(jnp.float32)
    running = jnp.zeros_like(source)
    weight_sum = jnp.zeros((length, 1), jnp.float32)
    for offset in range(window):
        earlier = jnp.pad(source, ((offset, 0), (0, 0)))[:length]
        earlier_docs = jnp.pad(doc_ids, (offset, 0), constant_values=-1)[:length]
        same_doc = (earlier_docs == doc_ids).astype(jnp.float32)[:, None]
        running = running + same_doc * earlier
        weight_sum = weight_sum + same_doc
    return running / weight_sum - source

def expert_sum(normed, routes, weight, expert_gate, expert_up, expert_down):
    flat_routes = routes.reshape(-1).astype(jnp.int32)
    entry_count = flat_routes.shape[0]
    sorted_entries = jnp.argsort(flat_routes, stable=True).astype(jnp.int32)
    counts = lax.optimization_barrier(jnp.sum((flat_routes[:, None] == jnp.arange(EXPERTS, dtype=jnp.int32)[None, :]).astype(jnp.int32), axis=0))
    starts = (jnp.cumsum(counts) - counts).astype(jnp.int32)
    load_limit = TOKENS // (ROWS // 2) * SLOTS
    entries_padded = jnp.concatenate([sorted_entries, jnp.full((load_limit,), entry_count, jnp.int32)])
    flat_weight = jnp.concatenate([weight.reshape(-1), jnp.zeros((1,), jnp.float32)])
    padded_rows = jnp.concatenate([normed, jnp.zeros((1, normed.shape[1]), normed.dtype)], axis=0)

    def expert_step(routed_sum, expert):
        entry_ids = lax.dynamic_slice_in_dim(entries_padded, starts[expert], load_limit)
        live_mask = jnp.arange(load_limit, dtype=jnp.int32) < counts[expert]
        entry_ids = jnp.where(live_mask, entry_ids, entry_count).astype(jnp.int32)
        token_ids = (entry_ids // TOPK).astype(jnp.int32)
        gathered = padded_rows[token_ids]
        gate_out = jnp.dot(gathered, expert_gate[expert], preferred_element_type=jnp.float32)
        up_out = jnp.dot(gathered, expert_up[expert], preferred_element_type=jnp.float32)
        hidden = (jax.nn.silu(gate_out) * up_out).astype(jnp.bfloat16)
        result = jnp.dot(hidden, expert_down[expert], preferred_element_type=jnp.float32).astype(jnp.bfloat16)
        term = flat_weight[entry_ids][:, None] * result.astype(jnp.float32)
        return (routed_sum.at[token_ids].add(term), None)
    routed_sum = jnp.zeros((TOKENS + 1, normed.shape[1]), jnp.float32)
    routed_sum, unused = lax.scan(expert_step, routed_sum, jnp.arange(EXPERTS, dtype=jnp.int32))
    return routed_sum[:TOKENS]

def reference(residual, pool_input, doc_ids, pool_map, pool_scale, out_weight, mix_gain, mix_shift, group_router, expert_router, expert_gate, expert_up, expert_down, routes, ffn_gain, ffn_shift):
    mixed_parts = []
    for group_index in range(PGROUPS):
        columns = slice(group_index * GW, (group_index + 1) * GW)
        pooled = pool_group(pool_input[:, columns], doc_ids, 2 ** (group_index + 1)).astype(jnp.bfloat16)
        mapped = jnp.dot(pooled, pool_map[group_index], preferred_element_type=jnp.float32) * pool_scale[columns]
        mixed_parts.append(mapped.astype(jnp.bfloat16))
    mixed = jnp.concatenate(mixed_parts, axis=1)
    branch = jnp.dot(mixed, out_weight, preferred_element_type=jnp.float32)
    normed = layer_norm(skip_scale * residual.astype(jnp.float32) + branch, mix_gain, mix_shift).astype(jnp.bfloat16)
    weight = route_weights(normed, routes, group_router, expert_router)
    routed = expert_sum(normed, routes, weight, expert_gate, expert_up, expert_down)
    return layer_norm(skip_scale * normed.astype(jnp.float32) + routed, ffn_gain, ffn_shift).astype(jnp.bfloat16)
```

```python
import jax
import jax.numpy as jnp
from jax import lax
from jax.experimental import pallas as pl
from jax.experimental.pallas import tpu as pltpu
from jax.sharding import PartitionSpec as P

skip_scale = 2.0**0.5
epsilon = 1e-05
f32 = jnp.float32
bf16 = jnp.bfloat16

TAIL = 16
BLK = 128
CHANNELS = 256
HALF = 128
SLOTS = 512
EXPERTS = 64
WIDTH = 2048


def whole(memory_space=pltpu.VMEM):
    return pl.BlockSpec(memory_space=memory_space)


def dot(a, b, dims=((1,), (0,)), **kw):
    return lax.dot_general(a, b, (dims, ((), ())), preferred_element_type=f32, **kw)


def pool_kernel(info, x, tail, docs, pool_map, scale, out0, out1, out2, out3, xs, ds):
    tp, sp = info[0], info[1]
    xs[0 : BLK - TAIL, :] = jnp.zeros((BLK - TAIL, CHANNELS), bf16)
    xs[BLK - TAIL : BLK, :] = tail[0:TAIL, :]
    xs[BLK:, :] = x[...]
    tail_docs = tail[TAIL : TAIL + 1, CHANNELS - BLK :].astype(f32)
    ds[0:1, :] = jnp.where(sp == 0, -1.0, tail_docs)
    ds[1:9, :] = docs[...].astype(f32)
    window = jnp.left_shift(jnp.int32(2), tp)
    t_pos = lax.broadcasted_iota(jnp.int32, (BLK, BLK), 0)
    s_pos = lax.broadcasted_iota(jnp.int32, (BLK, BLK), 1)
    back = t_pos - s_pos
    in_cur = (back >= 0) & (back < window)
    in_prev = back + BLK < window
    group = pool_map[0]
    for d, out in enumerate((out0, out1, out2, out3)):
        owner = (tp + d) % 4
        for part in range(2):
            b = owner * 2 + part
            row = pl.multiple_of(b * BLK, BLK)
            prev_docs = ds[pl.ds(b, 1), :]
            cur_docs = ds[pl.ds(b + 1, 1), :]
            own_docs = jnp.transpose(jnp.broadcast_to(cur_docs, (BLK, BLK)))
            keep_cur = jnp.where(in_cur & (own_docs == cur_docs), 1.0, 0.0)
            keep_prev = jnp.where(in_prev & (own_docs == prev_docs), 1.0, 0.0)
            count = jnp.sum(keep_cur + keep_prev, axis=1, keepdims=True)
            cur = xs[pl.ds(row + BLK, BLK), :]
            prev = xs[pl.ds(row, BLK), :]
            running = dot(keep_cur.astype(bf16), cur) + dot(keep_prev.astype(bf16), prev)
            pooled = (running / count - cur.astype(f32)).astype(bf16)
            mixed = dot(pooled, group) * scale[...]
            out[part * BLK : (part + 1) * BLK, :] = mixed.astype(bf16)


def pool(info, x, tail, docs, pool_map, scale):
    rows = x.shape[0]
    shape = jax.ShapeDtypeStruct((rows // 4, CHANNELS), bf16)
    return pl.pallas_call(
        pool_kernel,
        out_shape=[shape] * 4,
        in_specs=[whole(pltpu.SMEM)] + [whole()] * 5,
        out_specs=[whole()] * 4,
        scratch_shapes=[pltpu.VMEM((rows + BLK, CHANNELS), bf16), pltpu.VMEM((16, BLK), f32)],
        name="pool",
    )(info, x, tail, docs, pool_map, scale)


def slot_kernel(routes, gather, spread):
    strict = (
        lax.broadcasted_iota(jnp.int32, (HALF, HALF), 1)
        < lax.broadcasted_iota(jnp.int32, (HALF, HALF), 0)
    )
    strict = jnp.where(strict, 1.0, 0.0).astype(bf16)
    expert = lax.broadcasted_iota(jnp.int32, (HALF, EXPERTS), 1)
    slot = lax.broadcasted_iota(jnp.int32, (HALF, SLOTS), 1)
    for h in range(2):
        chosen = routes[h * HALF : (h + 1) * HALF, :]
        first, second = chosen[:, 0:1], chosen[:, 1:2]
        hot0 = jnp.where(expert == first, 1.0, 0.0)
        hot1 = jnp.where(expert == second, 1.0, 0.0)
        before0 = dot(strict, hot0.astype(bf16))
        before1 = dot(strict, hot1.astype(bf16)) + jnp.sum(hot0, axis=0, keepdims=True)
        rank0 = jnp.sum(before0 * hot0, axis=1, keepdims=True).astype(jnp.int32)
        rank1 = jnp.sum(before1 * hot1, axis=1, keepdims=True).astype(jnp.int32)
        hit = (slot == first * 8 + rank0) | (slot == second * 8 + rank1)
        hit = jnp.where(hit, 1.0, 0.0)
        spread[h] = hit.astype(bf16)
        gather[h] = jnp.transpose(hit).astype(bf16)


def slots(routes):
    return pl.pallas_call(
        slot_kernel,
        out_shape=[
            jax.ShapeDtypeStruct((2, SLOTS, HALF), bf16),
            jax.ShapeDtypeStruct((2, HALF, SLOTS), bf16),
        ],
        in_specs=[whole()],
        out_specs=[whole()] * 2,
        name="slots",
    )(routes)


def norm(values, gain, shift):
    mean = jnp.mean(values, axis=-1, keepdims=True)
    center = values - mean
    var = jnp.mean(center * center, axis=-1, keepdims=True)
    return center * lax.rsqrt(var + epsilon) * gain + shift


def mix_kernel(info, m0, m1, m2, m3, weight, residual, gain, shift, gather, normed_out, rows_out):
    tp = info[0]
    branch = None
    for d, m in enumerate((m0, m1, m2, m3)):
        group = (tp + 4 - d) % 4
        row = pl.multiple_of(group * CHANNELS, CHANNELS)
        term = dot(m[...], weight[pl.ds(row, CHANNELS), :])
        branch = term if branch is None else branch + term
    values = skip_scale * residual[...].astype(f32) + branch
    normed = norm(values, gain[...], shift[...]).astype(bf16)
    normed_out[...] = normed
    rows_out[...] = dot(gather[0], normed).astype(bf16)


def mix(half, info, parts, weight, residual, gain, shift, gather):
    def rows_of(width):
        return pl.BlockSpec((HALF, width), lambda i: (half, 0))

    def full(*shape):
        return pl.BlockSpec(shape, lambda i: (0,) * len(shape))

    return pl.pallas_call(
        mix_kernel,
        grid=(1,),
        out_shape=[
            jax.ShapeDtypeStruct((HALF, WIDTH), bf16),
            jax.ShapeDtypeStruct((SLOTS, WIDTH), bf16),
        ],
        in_specs=[whole(pltpu.SMEM)]
        + [rows_of(CHANNELS)] * 4
        + [
            full(*weight.shape),
            rows_of(WIDTH),
            full(1, WIDTH),
            full(1, WIDTH),
            pl.BlockSpec((1, SLOTS, HALF), lambda i: (half, 0, 0)),
        ],
        out_specs=[full(HALF, WIDTH), full(SLOTS, WIDTH)],
        name="mix",
    )(info, *parts, weight, residual, gain, shift, gather)


def weight_kernel(normed, group_router, expert_router, spread, high_out, low_out):
    rows = normed[...]
    group_logits = dot(rows, group_router[...])
    expert_logits = dot(rows, expert_router[...])
    group_exp = jnp.exp(group_logits)
    group_prob = group_exp / jnp.sum(group_exp, axis=1, keepdims=True)
    slot = lax.broadcasted_iota(jnp.int32, (EXPERTS, SLOTS), 1)
    expert = lax.broadcasted_iota(jnp.int32, (EXPERTS, SLOTS), 0)
    widen = jnp.where(slot // 8 == expert, 1.0, 0.0)
    slot = lax.broadcasted_iota(jnp.int32, (4, SLOTS), 1)
    group = lax.broadcasted_iota(jnp.int32, (4, SLOTS), 0)
    widen_group = jnp.where(slot // (SLOTS // 4) == group, 1.0, 0.0)
    logits = dot(expert_logits, widen, precision=lax.Precision.HIGHEST)
    share = dot(group_prob, widen_group, precision=lax.Precision.HIGHEST)
    hit = spread[0] > 0
    picked_exp = jnp.where(hit, jnp.exp(logits), 0.0)
    pair_share = picked_exp / jnp.sum(picked_exp, axis=1, keepdims=True)
    weight = jnp.where(hit, share * pair_share, 0.0)
    high = weight.astype(bf16)
    high_out[...] = high
    low_out[...] = (weight - high.astype(f32)).astype(bf16)


def weights(half, normed, group_router, expert_router, spread):
    def full(*shape):
        return pl.BlockSpec(shape, lambda i: (0,) * len(shape))

    return pl.pallas_call(
        weight_kernel,
        grid=(1,),
        out_shape=[jax.ShapeDtypeStruct((HALF, SLOTS), bf16)] * 2,
        in_specs=[
            full(HALF, WIDTH),
            full(*group_router.shape),
            full(*expert_router.shape),
            pl.BlockSpec((1, HALF, SLOTS), lambda i: (half, 0, 0)),
        ],
        out_specs=[full(HALF, SLOTS)] * 2,
        name="weights",
    )(normed, group_router, expert_router, spread)


def finish_kernel(high, low, returned, normed, gain, shift, *rest):
    out = rest[-1]
    routed = dot(high[...], returned[...]) + dot(low[...], returned[...])
    values = skip_scale * normed[...].astype(f32) + routed
    out[...] = norm(values, gain[...], shift[...]).astype(bf16)


def finish(half, high, low, returned, normed, gain, shift, base=None):
    def full(*shape):
        return pl.BlockSpec(shape, lambda i: (0,) * len(shape))

    operands = [high, low, returned, normed, gain, shift]
    in_specs = [full(*a.shape) for a in operands]
    aliases = {}
    if base is not None:
        operands.append(base)
        in_specs.append(pl.BlockSpec(memory_space=pl.ANY))
        aliases = {6: 0}
    return pl.pallas_call(
        finish_kernel,
        grid=(1,),
        out_shape=jax.ShapeDtypeStruct((2 * HALF, WIDTH), bf16),
        in_specs=in_specs,
        out_specs=pl.BlockSpec((HALF, WIDTH), lambda i: (half, 0)),
        input_output_aliases=aliases,
        name="finish",
    )(*operands)


def expert_ffn(arrived, expert_gate, expert_up, expert_down):
    gate_out = jnp.dot(arrived, expert_gate[0], preferred_element_type=f32)
    up_out = jnp.dot(arrived, expert_up[0], preferred_element_type=f32)
    hidden = (jax.nn.silu(gate_out) * up_out).astype(bf16)
    return jnp.dot(hidden, expert_down[0], preferred_element_type=f32).astype(bf16)


def exchange(rows):
    blocks = rows.reshape(EXPERTS, SLOTS // EXPERTS, WIDTH)
    moved = lax.all_to_all(blocks, "sp", split_axis=0, concat_axis=0, tiled=True)
    return moved.reshape(SLOTS, WIDTH)


def on_device(
    residual,
    pool_input,
    doc_ids,
    pool_map,
    pool_scale,
    out_weight,
    mix_gain,
    mix_shift,
    group_router,
    expert_router,
    expert_gate,
    expert_up,
    expert_down,
    routes,
    ffn_gain,
    ffn_shift,
):
    seq_rows = pool_input.shape[0]
    sp_count = lax.axis_size("sp")
    info = jnp.stack([lax.axis_index("tp"), lax.axis_index("sp")]).astype(jnp.int32)
    message = jnp.concatenate(
        [
            pool_input[seq_rows - TAIL :],
            doc_ids[seq_rows - CHANNELS :].astype(bf16)[None, :],
            jnp.zeros((TAIL - 1, CHANNELS), bf16),
        ],
        axis=0,
    )
    tail = lax.ppermute(message, "sp", [(i, i + 1) for i in range(sp_count - 1)])
    gather, spread = slots(routes)
    blocks = pool(
        info,
        pool_input,
        tail,
        doc_ids.reshape(seq_rows // BLK, BLK),
        pool_map,
        pool_scale[None, :],
    )
    parts = [blocks[0]] + [
        lax.ppermute(blocks[d], "tp", [(i, (i + d) % 4) for i in range(4)]) for d in range(1, 4)
    ]
    normed, arrived, high, low = [], [], [], []
    for h in range(2):
        rows, outgoing = mix(
            h, info, parts, out_weight, residual, mix_gain[None, :], mix_shift[None, :], gather
        )
        normed.append(rows)
        arrived.append(exchange(outgoing))
        split = weights(h, rows, group_router, expert_router, spread)
        high.append(split[0])
        low.append(split[1])
    result = None
    for h in range(2):
        returned = exchange(expert_ffn(arrived[h], expert_gate, expert_up, expert_down))
        result = finish(
            h, high[h], low[h], returned, normed[h], ffn_gain[None, :], ffn_shift[None, :], result
        )
    return result


def solution(mesh):
    in_specs = (
        P(("sp", "tp"), None),
        P("sp", "tp"),
        P("sp"),
        P("tp", None, None),
        P("tp"),
        P(),
        P(),
        P(),
        P(),
        P(),
        P("sp", None, None),
        P("sp", None, None),
        P("sp", None, None),
        P(("sp", "tp"), None),
        P(),
        P(),
    )
    out_specs = P(("sp", "tp"), None)
    return jax.shard_map(
        on_device, mesh=mesh, in_specs=in_specs, out_specs=out_specs, check_vma=False
    )
```

```python
import functools

import jax
import jax.numpy as jnp
from jax import lax
from jax.experimental import pallas as pl
from jax.experimental.pallas import tpu as pltpu
from jax.sharding import PartitionSpec as P

skip_scale = 2.0**0.5
epsilon = 1e-05
f32 = jnp.float32
bf16 = jnp.bfloat16

TAIL = 16
BLK = 128
CHANNELS = 256
HALF = 128
SLOTS = 512
EXPERTS = 64
WIDTH = 2048
CHUNKS = 4


VMEM = pl.BlockSpec(memory_space=pltpu.VMEM)
HBM = pl.BlockSpec(memory_space=pltpu.MemorySpace.HBM)
ROOM = pltpu.CompilerParams(vmem_limit_bytes=48 * 2**20)


def in_hbm(*arrays):
    held = [pltpu.with_memory_space_constraint(a, pltpu.MemorySpace.HBM) for a in arrays]
    return held if len(held) > 1 else held[0]


def dot(a, b, dims=((1,), (0,)), **kw):
    return lax.dot_general(a, b, (dims, ((), ())), preferred_element_type=f32, **kw)


def boundary_kernel(x, docs, out, last, sems):
    loads = [
        pltpu.make_async_copy(
            x.at[pl.ds(x.shape[0] - TAIL, TAIL), :], out.at[pl.ds(0, TAIL), :], sems.at[0]
        ),
        pltpu.make_async_copy(docs, last, sems.at[1]),
    ]
    for load in loads:
        load.start()
    out[TAIL:, BLK:] = jnp.zeros((TAIL, CHANNELS - BLK), bf16)
    loads[1].wait()
    ids = last[docs.shape[0] - 1 :, :].astype(f32).astype(bf16)
    out[TAIL:, 0:BLK] = jnp.broadcast_to(ids, (TAIL, BLK))
    loads[0].wait()


def boundary(x, docs):
    return pl.pallas_call(
        boundary_kernel,
        out_shape=jax.ShapeDtypeStruct((2 * TAIL, CHANNELS), bf16),
        in_specs=[HBM, HBM],
        out_specs=VMEM,
        scratch_shapes=[pltpu.VMEM(docs.shape, jnp.int32), pltpu.SemaphoreType.DMA((2,))],
        name="boundary",
        compiler_params=ROOM,
    )(*in_hbm(x, docs))


def pool_kernel(
    half, x, tail, docs_in, map_in, scale_in, out0, out1, out2, out3, xs, ds, docs, pool_map, scale, sems
):
    tp, sp = lax.axis_index("tp"), lax.axis_index("sp")
    loads = [
        pltpu.make_async_copy(docs_in, docs, sems.at[0]),
        pltpu.make_async_copy(x, xs.at[pl.ds(BLK, x.shape[0]), :], sems.at[1]),
        pltpu.make_async_copy(map_in, pool_map, sems.at[2]),
        pltpu.make_async_copy(scale_in, scale, sems.at[3]),
    ]
    for load in loads:
        load.start()
    xs[0 : BLK - TAIL, :] = jnp.zeros((BLK - TAIL, CHANNELS), bf16)
    xs[BLK - TAIL : BLK, :] = tail[0:TAIL, :]
    tail_docs = tail[TAIL : TAIL + 1, 0:BLK].astype(f32)
    ds[0:1, :] = jnp.where(sp == 0, -1.0, tail_docs)
    loads[0].wait()
    ds[1:9, :] = docs[...].astype(f32)
    window = jnp.left_shift(jnp.int32(2), tp)
    t_pos = lax.broadcasted_iota(jnp.int32, (BLK, BLK), 0)
    s_pos = lax.broadcasted_iota(jnp.int32, (BLK, BLK), 1)
    back = t_pos - s_pos
    in_cur = (back >= 0) & (back < window)
    in_prev = back + BLK < window
    kept = []
    for d in range(4):
        b = ((tp + d) % 4) * 2 + half
        prev_docs = ds[pl.ds(b, 1), :]
        cur_docs = ds[pl.ds(b + 1, 1), :]
        own_docs = jnp.transpose(jnp.broadcast_to(cur_docs, (BLK, BLK)))
        keep_cur = jnp.where(in_cur & (own_docs == cur_docs), 1.0, 0.0)
        keep_prev = jnp.where(in_prev & (own_docs == prev_docs), 1.0, 0.0)
        count = jnp.sum(keep_cur + keep_prev, axis=1, keepdims=True)
        kept.append((b, keep_cur.astype(bf16), keep_prev.astype(bf16), count))
    for load in loads[1:]:
        load.wait()
    group = pool_map[0]
    for (b, keep_cur, keep_prev, count), out in zip(kept, (out0, out1, out2, out3)):
        row = pl.multiple_of(b * BLK, BLK)
        cur = xs[pl.ds(row + BLK, BLK), :]
        prev = xs[pl.ds(row, BLK), :]
        running = dot(keep_cur, cur) + dot(keep_prev, prev)
        pooled = (running / count - cur.astype(f32)).astype(bf16)
        mixed = dot(pooled, group) * scale[...]
        out[...] = mixed.astype(bf16)


def pool(half, x, tail, docs, pool_map, scale):
    rows = x.shape[0]
    return pl.pallas_call(
        functools.partial(pool_kernel, half),
        out_shape=[jax.ShapeDtypeStruct((HALF, CHANNELS), bf16)] * 4,
        in_specs=[HBM, VMEM, HBM, HBM, HBM],
        out_specs=[VMEM] * 4,
        scratch_shapes=[
            pltpu.VMEM((rows + BLK, CHANNELS), bf16),
            pltpu.VMEM((16, BLK), f32),
            pltpu.VMEM(docs.shape, jnp.int32),
            pltpu.VMEM(pool_map.shape, bf16),
            pltpu.VMEM(scale.shape, f32),
            pltpu.SemaphoreType.DMA((4,)),
        ],
        name="pool",
        compiler_params=ROOM,
    )(in_hbm(x), tail, *in_hbm(docs, pool_map, scale))


def slots_of(chosen):
    strict = (
        lax.broadcasted_iota(jnp.int32, (HALF, HALF), 1)
        < lax.broadcasted_iota(jnp.int32, (HALF, HALF), 0)
    )
    strict = jnp.where(strict, 1.0, 0.0).astype(bf16)
    expert = lax.broadcasted_iota(jnp.int32, (HALF, EXPERTS), 1)
    slot = lax.broadcasted_iota(jnp.int32, (HALF, SLOTS), 1)
    first, second = chosen[:, 0:1], chosen[:, 1:2]
    hot0 = jnp.where(expert == first, 1.0, 0.0)
    hot1 = jnp.where(expert == second, 1.0, 0.0)
    before0 = dot(strict, hot0.astype(bf16))
    before1 = dot(strict, hot1.astype(bf16)) + jnp.sum(hot0, axis=0, keepdims=True)
    rank0 = jnp.sum(before0 * hot0, axis=1, keepdims=True).astype(jnp.int32)
    rank1 = jnp.sum(before1 * hot1, axis=1, keepdims=True).astype(jnp.int32)
    return slot == first * 8 + rank0, slot == second * 8 + rank1


def slot_kernel(routes, weight, gather, near_weight, sem):
    load = pltpu.make_async_copy(weight, near_weight, sem)
    load.start()
    for h in range(2):
        hit0, hit1 = slots_of(routes[h * HALF : (h + 1) * HALF, :])
        hit = jnp.where(hit0 | hit1, 1.0, 0.0)
        gather[h] = jnp.transpose(hit).astype(bf16)
    load.wait()


def slots(routes, weight):
    return pl.pallas_call(
        slot_kernel,
        out_shape=[
            jax.ShapeDtypeStruct((2, SLOTS, HALF), bf16),
            jax.ShapeDtypeStruct(weight.shape, bf16),
        ],
        in_specs=[VMEM, HBM],
        out_specs=[VMEM] * 2,
        scratch_shapes=[pltpu.SemaphoreType.DMA],
        name="slots",
        compiler_params=ROOM,
    )(routes, weight)


def norm(values, gain, shift):
    mean = jnp.mean(values, axis=-1, keepdims=True)
    center = values - mean
    var = jnp.mean(center * center, axis=-1, keepdims=True)
    return center * lax.rsqrt(var + epsilon) * gain + shift


def mix_kernel(
    half, m0, m1, m2, m3, weight, residual, gain, shift, gather, rows_out, res, rows, sems
):
    tp = lax.axis_index("tp")
    load = pltpu.make_async_copy(residual.at[pl.ds(half * HALF, HALF), :], res, sems.at[CHUNKS])
    load.start()
    branch = None
    for d, m in enumerate((m0, m1, m2, m3)):
        group = (tp + 4 - d) % 4
        row = pl.multiple_of(group * CHANNELS, CHANNELS)
        term = dot(m[...], weight[pl.ds(row, CHANNELS), :])
        branch = term if branch is None else branch + term
    load.wait()
    values = skip_scale * res[...].astype(f32) + branch
    normed = norm(values, gain[...], shift[...]).astype(bf16)
    stores = []
    for c in range(CHUNKS):
        part = slice(c * SLOTS // CHUNKS, (c + 1) * SLOTS // CHUNKS)
        rows[part, :] = dot(gather[half, part, :], normed).astype(bf16)
        stores.append(pltpu.make_async_copy(rows.at[part, :], rows_out.at[part, :], sems.at[c]))
        stores[-1].start()
    for store in stores:
        store.wait()


def mix(half, parts, weight, residual, gain, shift, gather):
    return pl.pallas_call(
        functools.partial(mix_kernel, half),
        out_shape=jax.ShapeDtypeStruct((SLOTS, WIDTH), bf16),
        in_specs=[VMEM] * 5 + [HBM] + [VMEM] * 3,
        out_specs=HBM,
        scratch_shapes=[
            pltpu.VMEM((HALF, WIDTH), bf16),
            pltpu.VMEM((SLOTS, WIDTH), bf16),
            pltpu.SemaphoreType.DMA((CHUNKS + 1,)),
        ],
        name="mix",
        compiler_params=ROOM,
    )(*parts, weight, in_hbm(residual), gain, shift, gather)


def weight_kernel(half, laid_out, group_router, expert_router, routes, normed, high_out, low_out):
    hit0, hit1 = slots_of(routes[half * HALF : (half + 1) * HALF, :])
    rows = dot(jnp.where(hit0, 1.0, 0.0).astype(bf16), laid_out[...]).astype(bf16)
    normed[...] = rows
    group_logits = dot(rows, group_router[...])
    expert_logits = dot(rows, expert_router[...])
    group_exp = jnp.exp(group_logits)
    group_prob = group_exp / jnp.sum(group_exp, axis=1, keepdims=True)
    slot = lax.broadcasted_iota(jnp.int32, (EXPERTS, SLOTS), 1)
    expert = lax.broadcasted_iota(jnp.int32, (EXPERTS, SLOTS), 0)
    widen = jnp.where(slot // 8 == expert, 1.0, 0.0)
    slot = lax.broadcasted_iota(jnp.int32, (4, SLOTS), 1)
    group = lax.broadcasted_iota(jnp.int32, (4, SLOTS), 0)
    widen_group = jnp.where(slot // (SLOTS // 4) == group, 1.0, 0.0)
    logits = dot(expert_logits, widen, precision=lax.Precision.HIGHEST)
    share = dot(group_prob, widen_group, precision=lax.Precision.HIGHEST)
    hit = hit0 | hit1
    picked_exp = jnp.where(hit, jnp.exp(logits), 0.0)
    pair_share = picked_exp / jnp.sum(picked_exp, axis=1, keepdims=True)
    weight = jnp.where(hit, share * pair_share, 0.0)
    high = weight.astype(bf16)
    high_out[...] = high
    low_out[...] = (weight - high.astype(f32)).astype(bf16)


def weights(half, laid_out, group_router, expert_router, routes):
    return pl.pallas_call(
        functools.partial(weight_kernel, half),
        out_shape=[jax.ShapeDtypeStruct((HALF, WIDTH), bf16)]
        + [jax.ShapeDtypeStruct((HALF, SLOTS), bf16)] * 2,
        in_specs=[VMEM] * 4,
        out_specs=[VMEM] * 3,
        name="weights",
    )(laid_out, group_router, expert_router, routes)


def finish_kernel(high, low, returned, normed, gain, shift, *rest):
    out = rest[-1]
    routed = dot(high[...], returned[...]) + dot(low[...], returned[...])
    values = skip_scale * normed[...].astype(f32) + routed
    out[...] = norm(values, gain[...], shift[...]).astype(bf16)


def finish(half, high, low, returned, normed, gain, shift, base=None):
    def full(*shape):
        return pl.BlockSpec(shape, lambda i: (0,) * len(shape))

    operands = [high, low, returned, normed, gain, shift]
    in_specs = [full(*a.shape) for a in operands]
    aliases = {}
    if base is not None:
        operands.append(base)
        in_specs.append(HBM)
        aliases = {6: 0}
    return pl.pallas_call(
        finish_kernel,
        grid=(1,),
        out_shape=jax.ShapeDtypeStruct((2 * HALF, WIDTH), bf16),
        in_specs=in_specs,
        out_specs=pl.BlockSpec((HALF, WIDTH), lambda i: (half, 0)),
        input_output_aliases=aliases,
        name="finish",
    )(*operands)


def expert_ffn(arrived, expert_gate, expert_up, expert_down):
    gate_out = jnp.dot(arrived, expert_gate[0], preferred_element_type=f32)
    up_out = jnp.dot(arrived, expert_up[0], preferred_element_type=f32)
    hidden = (jax.nn.silu(gate_out) * up_out).astype(bf16)
    return jnp.dot(hidden, expert_down[0], preferred_element_type=f32).astype(bf16)


def exchange(rows):
    blocks = rows.reshape(EXPERTS, SLOTS // EXPERTS, WIDTH)
    moved = lax.all_to_all(blocks, "sp", split_axis=0, concat_axis=0, tiled=True)
    return moved.reshape(SLOTS, WIDTH)


def on_device(
    residual,
    pool_input,
    doc_ids,
    pool_map,
    pool_scale,
    out_weight,
    mix_gain,
    mix_shift,
    group_router,
    expert_router,
    expert_gate,
    expert_up,
    expert_down,
    routes,
    ffn_gain,
    ffn_shift,
):
    sp_count = lax.axis_size("sp")
    docs = doc_ids.reshape(doc_ids.shape[0] // BLK, BLK)
    message = boundary(pool_input, docs)
    tail = lax.ppermute(message, "sp", [(i, i + 1) for i in range(sp_count - 1)])
    gather, near_weight = slots(routes, out_weight)
    near_weight = pltpu.with_memory_space_constraint(near_weight, pltpu.VMEM)
    parts = []
    for h in range(2):
        blocks = pool(h, pool_input, tail, docs, pool_map, pool_scale[None, :])
        parts.append(
            [blocks[0]]
            + [
                lax.ppermute(blocks[d], "tp", [(i, (i + d) % 4) for i in range(4)])
                for d in range(1, 4)
            ]
        )
    arrived, kept = [], []
    for h in range(2):
        outgoing = mix(
            h,
            parts[h],
            (near_weight, out_weight)[h],
            residual,
            mix_gain[None, :],
            mix_shift[None, :],
            gather,
        )
        arrived.append(exchange(outgoing))
        kept.append(weights(h, outgoing, group_router, expert_router, routes))
    result = None
    for h in range(2):
        returned = exchange(expert_ffn(arrived[h], expert_gate, expert_up, expert_down))
        normed, high, low = kept[h]
        result = finish(
            h, high, low, returned, normed, ffn_gain[None, :], ffn_shift[None, :], result
        )
    return result


def solution(mesh):
    in_specs = (
        P(("sp", "tp"), None),
        P("sp", "tp"),
        P("sp"),
        P("tp", None, None),
        P("tp"),
        P(),
        P(),
        P(),
        P(),
        P(),
        P("sp", None, None),
        P("sp", None, None),
        P("sp", None, None),
        P(("sp", "tp"), None),
        P(),
        P(),
    )
    out_specs = P(("sp", "tp"), None)
    return jax.shard_map(
        on_device, mesh=mesh, in_specs=in_specs, out_specs=out_specs, check_vma=False
    )
```

```python
import functools

import jax
import jax.numpy as jnp
from jax import lax
from jax.experimental import pallas as pl
from jax.experimental.pallas import tpu as pltpu
from jax.sharding import PartitionSpec as P

skip_scale = 2.0**0.5
epsilon = 1e-05
f32 = jnp.float32
bf16 = jnp.bfloat16

TAIL = 16
BLK = 128
CHANNELS = 256
HALF = 128
SLOTS = 512
EXPERTS = 64
WIDTH = 2048
CHUNKS = 4


VMEM = pl.BlockSpec(memory_space=pltpu.VMEM)
HBM = pl.BlockSpec(memory_space=pltpu.MemorySpace.HBM)
ROOM = pltpu.CompilerParams(vmem_limit_bytes=48 * 2**20)


def in_hbm(*arrays):
    held = [pltpu.with_memory_space_constraint(a, pltpu.MemorySpace.HBM) for a in arrays]
    return held if len(held) > 1 else held[0]


def dot(a, b, dims=((1,), (0,)), **kw):
    return lax.dot_general(a, b, (dims, ((), ())), preferred_element_type=f32, **kw)


def pool_kernel(half, *refs):
    if half == 0:
        tail, refs = refs[0], refs[1:]
    x, docs_in, map_in, scale_in, out0, out1, out2, out3 = refs[:8]
    xs, ds, docs, pool_map, scale, sems = refs[-6:]
    tp, sp = lax.axis_index("tp"), lax.axis_index("sp")
    loads = [
        pltpu.make_async_copy(docs_in, docs, sems.at[0]),
        pltpu.make_async_copy(x, xs.at[pl.ds(BLK, x.shape[0]), :], sems.at[1]),
        pltpu.make_async_copy(map_in, pool_map, sems.at[2]),
        pltpu.make_async_copy(scale_in, scale, sems.at[3]),
    ]
    for load in loads:
        load.start()
    if half == 0:
        xs[0 : BLK - TAIL, :] = jnp.zeros((BLK - TAIL, CHANNELS), bf16)
        xs[BLK - TAIL : BLK, :] = tail[0:TAIL, :]
        tail_docs = tail[TAIL : TAIL + 1, 0:BLK].astype(f32)
        ds[0:1, :] = jnp.where(sp == 0, -1.0, tail_docs)
    loads[0].wait()
    ds[1:9, :] = docs[...].astype(f32)
    window = jnp.left_shift(jnp.int32(2), tp)
    t_pos = lax.broadcasted_iota(jnp.int32, (BLK, BLK), 0)
    s_pos = lax.broadcasted_iota(jnp.int32, (BLK, BLK), 1)
    back = t_pos - s_pos
    in_cur = (back >= 0) & (back < window)
    in_prev = back + BLK < window
    kept = []
    for d in range(4):
        b = ((tp + d) % 4) * 2 + half
        prev_docs = ds[pl.ds(b, 1), :]
        cur_docs = ds[pl.ds(b + 1, 1), :]
        own_docs = jnp.transpose(jnp.broadcast_to(cur_docs, (BLK, BLK)))
        keep_cur = jnp.where(in_cur & (own_docs == cur_docs), 1.0, 0.0)
        keep_prev = jnp.where(in_prev & (own_docs == prev_docs), 1.0, 0.0)
        count = jnp.sum(keep_cur + keep_prev, axis=1, keepdims=True)
        kept.append((b, keep_cur.astype(bf16), keep_prev.astype(bf16), count))
    for load in loads[1:]:
        load.wait()
    group = pool_map[0]
    for (b, keep_cur, keep_prev, count), out in zip(kept, (out0, out1, out2, out3)):
        row = pl.multiple_of(b * BLK, BLK)
        cur = xs[pl.ds(row + BLK, BLK), :]
        prev = xs[pl.ds(row, BLK), :]
        running = dot(keep_cur, cur) + dot(keep_prev, prev)
        pooled = (running / count - cur.astype(f32)).astype(bf16)
        mixed = dot(pooled, group) * scale[...]
        out[...] = mixed.astype(bf16)
    if half == 1:
        message = refs[8]
        message[0:TAIL, :] = xs[BLK + x.shape[0] - TAIL :, :]
        message[TAIL:, 0:BLK] = jnp.broadcast_to(ds[8:9, :], (TAIL, BLK)).astype(bf16)
        message[TAIL:, BLK:] = jnp.zeros((TAIL, CHANNELS - BLK), bf16)


def pool(half, x, docs, pool_map, scale, tail=None):
    rows = x.shape[0]
    shapes = [jax.ShapeDtypeStruct((HALF, CHANNELS), bf16)] * 4
    if half == 1:
        shapes.append(jax.ShapeDtypeStruct((2 * TAIL, CHANNELS), bf16))
    first = [] if tail is None else [tail]
    return pl.pallas_call(
        functools.partial(pool_kernel, half),
        out_shape=shapes,
        in_specs=[VMEM] * len(first) + [HBM] * 4,
        out_specs=[VMEM] * len(shapes),
        scratch_shapes=[
            pltpu.VMEM((rows + BLK, CHANNELS), bf16),
            pltpu.VMEM((16, BLK), f32),
            pltpu.VMEM(docs.shape, jnp.int32),
            pltpu.VMEM(pool_map.shape, bf16),
            pltpu.VMEM(scale.shape, f32),
            pltpu.SemaphoreType.DMA((4,)),
        ],
        name="pool",
        compiler_params=ROOM,
    )(*first, *in_hbm(x, docs, pool_map, scale))


def slots_of(chosen):
    strict = (
        lax.broadcasted_iota(jnp.int32, (HALF, HALF), 1)
        < lax.broadcasted_iota(jnp.int32, (HALF, HALF), 0)
    )
    strict = jnp.where(strict, 1.0, 0.0).astype(bf16)
    expert = lax.broadcasted_iota(jnp.int32, (HALF, EXPERTS), 1)
    slot = lax.broadcasted_iota(jnp.int32, (HALF, SLOTS), 1)
    first, second = chosen[:, 0:1], chosen[:, 1:2]
    hot0 = jnp.where(expert == first, 1.0, 0.0)
    hot1 = jnp.where(expert == second, 1.0, 0.0)
    before0 = dot(strict, hot0.astype(bf16))
    before1 = dot(strict, hot1.astype(bf16)) + jnp.sum(hot0, axis=0, keepdims=True)
    rank0 = jnp.sum(before0 * hot0, axis=1, keepdims=True).astype(jnp.int32)
    rank1 = jnp.sum(before1 * hot1, axis=1, keepdims=True).astype(jnp.int32)
    return slot == first * 8 + rank0, slot == second * 8 + rank1


def slot_kernel(routes, weight, gather, near_weight, sem):
    load = pltpu.make_async_copy(weight, near_weight, sem)
    load.start()
    for h in range(2):
        hit0, hit1 = slots_of(routes[h * HALF : (h + 1) * HALF, :])
        hit = jnp.where(hit0 | hit1, 1.0, 0.0)
        gather[h] = jnp.transpose(hit).astype(bf16)
    load.wait()


def slots(routes, weight):
    return pl.pallas_call(
        slot_kernel,
        out_shape=[
            jax.ShapeDtypeStruct((2, SLOTS, HALF), bf16),
            jax.ShapeDtypeStruct(weight.shape, bf16),
        ],
        in_specs=[VMEM, HBM],
        out_specs=[VMEM] * 2,
        scratch_shapes=[pltpu.SemaphoreType.DMA],
        name="slots",
        compiler_params=ROOM,
    )(routes, weight)


def norm(values, gain, shift):
    mean = jnp.mean(values, axis=-1, keepdims=True)
    center = values - mean
    var = jnp.mean(center * center, axis=-1, keepdims=True)
    return center * lax.rsqrt(var + epsilon) * gain + shift


def mix_kernel(
    half, m0, m1, m2, m3, weight, residual, gain, shift, gather, rows_out, res, rows, sems
):
    tp = lax.axis_index("tp")
    load = pltpu.make_async_copy(residual.at[pl.ds(half * HALF, HALF), :], res, sems.at[CHUNKS])
    load.start()
    branch = None
    for d, m in enumerate((m0, m1, m2, m3)):
        group = (tp + 4 - d) % 4
        row = pl.multiple_of(group * CHANNELS, CHANNELS)
        term = dot(m[...], weight[pl.ds(row, CHANNELS), :])
        branch = term if branch is None else branch + term
    load.wait()
    values = skip_scale * res[...].astype(f32) + branch
    normed = norm(values, gain[...], shift[...]).astype(bf16)
    stores = []
    for c in range(CHUNKS):
        part = slice(c * SLOTS // CHUNKS, (c + 1) * SLOTS // CHUNKS)
        rows[part, :] = dot(gather[half, part, :], normed).astype(bf16)
        stores.append(pltpu.make_async_copy(rows.at[part, :], rows_out.at[part, :], sems.at[c]))
        stores[-1].start()
    for store in stores:
        store.wait()


def mix(half, parts, weight, residual, gain, shift, gather):
    return pl.pallas_call(
        functools.partial(mix_kernel, half),
        out_shape=jax.ShapeDtypeStruct((SLOTS, WIDTH), bf16),
        in_specs=[VMEM] * 5 + [HBM] + [VMEM] * 3,
        out_specs=HBM,
        scratch_shapes=[
            pltpu.VMEM((HALF, WIDTH), bf16),
            pltpu.VMEM((SLOTS, WIDTH), bf16),
            pltpu.SemaphoreType.DMA((CHUNKS + 1,)),
        ],
        name="mix",
        compiler_params=ROOM,
    )(*parts, weight, in_hbm(residual), gain, shift, gather)


def weight_kernel(half, laid_out, group_router, expert_router, routes, normed, split):
    hit0, hit1 = slots_of(routes[half * HALF : (half + 1) * HALF, :])
    rows = dot(jnp.where(hit0, 1.0, 0.0).astype(bf16), laid_out[...]).astype(bf16)
    normed[...] = rows
    group_logits = dot(rows, group_router[...])
    expert_logits = dot(rows, expert_router[...])
    group_exp = jnp.exp(group_logits)
    group_prob = group_exp / jnp.sum(group_exp, axis=1, keepdims=True)
    slot = lax.broadcasted_iota(jnp.int32, (EXPERTS, SLOTS), 1)
    expert = lax.broadcasted_iota(jnp.int32, (EXPERTS, SLOTS), 0)
    widen = jnp.where(slot // 8 == expert, 1.0, 0.0)
    slot = lax.broadcasted_iota(jnp.int32, (4, SLOTS), 1)
    group = lax.broadcasted_iota(jnp.int32, (4, SLOTS), 0)
    widen_group = jnp.where(slot // (SLOTS // 4) == group, 1.0, 0.0)
    logits = dot(expert_logits, widen, precision=lax.Precision.HIGHEST)
    share = dot(group_prob, widen_group, precision=lax.Precision.HIGHEST)
    hit = hit0 | hit1
    picked_exp = jnp.where(hit, jnp.exp(logits), 0.0)
    pair_share = picked_exp / jnp.sum(picked_exp, axis=1, keepdims=True)
    weight = jnp.where(hit, share * pair_share, 0.0)
    high = weight.astype(bf16)
    split[0:HALF, :] = high
    split[HALF:, :] = (weight - high.astype(f32)).astype(bf16)


def weights(half, laid_out, group_router, expert_router, routes):
    return pl.pallas_call(
        functools.partial(weight_kernel, half),
        out_shape=[
            jax.ShapeDtypeStruct((HALF, WIDTH), bf16),
            jax.ShapeDtypeStruct((2 * HALF, SLOTS), bf16),
        ],
        in_specs=[VMEM] * 4,
        out_specs=[VMEM] * 2,
        name="weights",
    )(laid_out, group_router, expert_router, routes)


def finish_kernel(split, returned, normed, gain, shift, *rest):
    out = rest[-1]
    both = dot(split[...], returned[...])
    routed = both[0:HALF, :] + both[HALF:, :]
    values = skip_scale * normed[...].astype(f32) + routed
    out[...] = norm(values, gain[...], shift[...]).astype(bf16)


def finish(half, split, returned, normed, gain, shift, base=None):
    def full(*shape):
        return pl.BlockSpec(shape, lambda i: (0,) * len(shape))

    operands = [split, returned, normed, gain, shift]
    in_specs = [full(*a.shape) for a in operands]
    aliases = {}
    if base is not None:
        operands.append(base)
        in_specs.append(HBM)
        aliases = {5: 0}
    return pl.pallas_call(
        finish_kernel,
        grid=(1,),
        out_shape=jax.ShapeDtypeStruct((2 * HALF, WIDTH), bf16),
        in_specs=in_specs,
        out_specs=pl.BlockSpec((HALF, WIDTH), lambda i: (half, 0)),
        input_output_aliases=aliases,
        name="finish",
    )(*operands)


def expert_ffn(arrived, expert_gate, expert_up, expert_down):
    gate_out = jnp.dot(arrived, expert_gate[0], preferred_element_type=f32)
    up_out = jnp.dot(arrived, expert_up[0], preferred_element_type=f32)
    hidden = (jax.nn.silu(gate_out) * up_out).astype(bf16)
    return jnp.dot(hidden, expert_down[0], preferred_element_type=f32).astype(bf16)


def exchange(rows):
    blocks = rows.reshape(EXPERTS, SLOTS // EXPERTS, WIDTH)
    moved = lax.all_to_all(blocks, "sp", split_axis=0, concat_axis=0, tiled=True)
    return moved.reshape(SLOTS, WIDTH)


def on_device(
    residual,
    pool_input,
    doc_ids,
    pool_map,
    pool_scale,
    out_weight,
    mix_gain,
    mix_shift,
    group_router,
    expert_router,
    expert_gate,
    expert_up,
    expert_down,
    routes,
    ffn_gain,
    ffn_shift,
):
    sp_count = lax.axis_size("sp")
    docs = doc_ids.reshape(doc_ids.shape[0] // BLK, BLK)
    inputs = (pool_input, docs, pool_map, pool_scale[None, :])
    parts, tail = {}, None
    for h in (1, 0):
        blocks = pool(h, *inputs, tail=tail)
        parts[h] = [blocks[0]] + [
            lax.ppermute(blocks[d], "tp", [(i, (i + d) % 4) for i in range(4)])
            for d in range(1, 4)
        ]
        if h == 1:
            tail = lax.ppermute(blocks[4], "sp", [(i, i + 1) for i in range(sp_count - 1)])
            gather, near_weight = slots(routes, out_weight)
            near_weight = pltpu.with_memory_space_constraint(near_weight, pltpu.VMEM)
    arrived, kept = {}, {}
    for h in (1, 0):
        outgoing = mix(
            h,
            parts[h],
            (out_weight, near_weight)[h],
            residual,
            mix_gain[None, :],
            mix_shift[None, :],
            gather,
        )
        arrived[h] = exchange(outgoing)
        kept[h] = weights(h, outgoing, group_router, expert_router, routes)
    result = None
    for h in (1, 0):
        returned = exchange(expert_ffn(arrived[h], expert_gate, expert_up, expert_down))
        normed, split = kept[h]
        result = finish(
            h, split, returned, normed, ffn_gain[None, :], ffn_shift[None, :], result
        )
    return result


def solution(mesh):
    in_specs = (
        P(("sp", "tp"), None),
        P("sp", "tp"),
        P("sp"),
        P("tp", None, None),
        P("tp"),
        P(),
        P(),
        P(),
        P(),
        P(),
        P("sp", None, None),
        P("sp", None, None),
        P("sp", None, None),
        P(("sp", "tp"), None),
        P(),
        P(),
    )
    out_specs = P(("sp", "tp"), None)
    return jax.shard_map(
        on_device, mesh=mesh, in_specs=in_specs, out_specs=out_specs, check_vma=False
    )
```

```python
import functools

import jax
import jax.numpy as jnp
from jax import lax
from jax.experimental import pallas as pl
from jax.experimental.pallas import tpu as pltpu
from jax.sharding import PartitionSpec as P

skip_scale = 2.0**0.5
epsilon = 1e-05
f32 = jnp.float32
bf16 = jnp.bfloat16

TAIL = 16
BLK = 128
CHANNELS = 256
HALF = 128
SLOTS = 512
EXPERTS = 64
WIDTH = 2048
CHUNKS = 4


VMEM = pl.BlockSpec(memory_space=pltpu.VMEM)
HBM = pl.BlockSpec(memory_space=pltpu.MemorySpace.HBM)
ROOM = pltpu.CompilerParams(vmem_limit_bytes=48 * 2**20)


def in_hbm(*arrays):
    held = [pltpu.with_memory_space_constraint(a, pltpu.MemorySpace.HBM) for a in arrays]
    return held if len(held) > 1 else held[0]


def dot(a, b, dims=((1,), (0,)), **kw):
    return lax.dot_general(a, b, (dims, ((), ())), preferred_element_type=f32, **kw)


def pool_kernel(half, *refs):
    if half == 0:
        tail, refs = refs[0], refs[1:]
    else:
        weight, refs = refs[0], refs[1:]
    x, docs_in, map_in, scale_in, out0, out1, out2, out3 = refs[:8]
    xs, ds, docs, pool_map, scale, sems = refs[-6:]
    tp, sp = lax.axis_index("tp"), lax.axis_index("sp")
    loads = [
        pltpu.make_async_copy(docs_in, docs, sems.at[0]),
        pltpu.make_async_copy(x, xs.at[pl.ds(BLK, x.shape[0]), :], sems.at[1]),
        pltpu.make_async_copy(map_in, pool_map, sems.at[2]),
        pltpu.make_async_copy(scale_in, scale, sems.at[3]),
    ]
    for load in loads:
        load.start()
    if half == 1:
        fetch = pltpu.make_async_copy(weight, refs[9], sems.at[4])
        fetch.start()
    if half == 0:
        xs[0 : BLK - TAIL, :] = jnp.zeros((BLK - TAIL, CHANNELS), bf16)
        xs[BLK - TAIL : BLK, :] = tail[0:TAIL, :]
        tail_docs = tail[TAIL : TAIL + 1, 0:BLK].astype(f32)
        ds[0:1, :] = jnp.where(sp == 0, -1.0, tail_docs)
    loads[0].wait()
    ds[1:9, :] = docs[...].astype(f32)
    window = jnp.left_shift(jnp.int32(2), tp)
    t_pos = lax.broadcasted_iota(jnp.int32, (BLK, BLK), 0)
    s_pos = lax.broadcasted_iota(jnp.int32, (BLK, BLK), 1)
    back = t_pos - s_pos
    in_cur = (back >= 0) & (back < window)
    in_prev = back + BLK < window
    kept = []
    for d in range(4):
        b = ((tp + d) % 4) * 2 + half
        prev_docs = ds[pl.ds(b, 1), :]
        cur_docs = ds[pl.ds(b + 1, 1), :]
        own_docs = jnp.transpose(jnp.broadcast_to(cur_docs, (BLK, BLK)))
        keep_cur = jnp.where(in_cur & (own_docs == cur_docs), 1.0, 0.0)
        keep_prev = jnp.where(in_prev & (own_docs == prev_docs), 1.0, 0.0)
        count = jnp.sum(keep_cur + keep_prev, axis=1, keepdims=True)
        kept.append((b, keep_cur.astype(bf16), keep_prev.astype(bf16), count))
    for load in loads[1:]:
        load.wait()
    group = pool_map[0]
    for (b, keep_cur, keep_prev, count), out in zip(kept, (out0, out1, out2, out3)):
        row = pl.multiple_of(b * BLK, BLK)
        cur = xs[pl.ds(row + BLK, BLK), :]
        prev = xs[pl.ds(row, BLK), :]
        running = dot(keep_cur, cur) + dot(keep_prev, prev)
        pooled = (running / count - cur.astype(f32)).astype(bf16)
        mixed = dot(pooled, group) * scale[...]
        out[...] = mixed.astype(bf16)
    if half == 1:
        message = refs[8]
        message[0:TAIL, :] = xs[BLK + x.shape[0] - TAIL :, :]
        message[TAIL:, 0:BLK] = jnp.broadcast_to(ds[8:9, :], (TAIL, BLK)).astype(bf16)
        message[TAIL:, BLK:] = jnp.zeros((TAIL, CHANNELS - BLK), bf16)
        fetch.wait()


def pool(half, x, docs, pool_map, scale, tail=None, weight=None):
    rows = x.shape[0]
    shapes = [jax.ShapeDtypeStruct((HALF, CHANNELS), bf16)] * 4
    if half == 1:
        shapes.append(jax.ShapeDtypeStruct((2 * TAIL, CHANNELS), bf16))
        shapes.append(jax.ShapeDtypeStruct(weight.shape, bf16))
    first = tail if half == 0 else in_hbm(weight)
    return pl.pallas_call(
        functools.partial(pool_kernel, half),
        out_shape=shapes,
        in_specs=[VMEM if half == 0 else HBM] + [HBM] * 4,
        out_specs=[VMEM] * len(shapes),
        scratch_shapes=[
            pltpu.VMEM((rows + BLK, CHANNELS), bf16),
            pltpu.VMEM((16, BLK), f32),
            pltpu.VMEM(docs.shape, jnp.int32),
            pltpu.VMEM(pool_map.shape, bf16),
            pltpu.VMEM(scale.shape, f32),
            pltpu.SemaphoreType.DMA((5,)),
        ],
        name="pool",
        compiler_params=ROOM,
    )(first, *in_hbm(x, docs, pool_map, scale))


def slots_of(routes, half):
    def column(k):
        row = routes[k : k + 1, half * HALF : (half + 1) * HALF].astype(f32)
        return jnp.transpose(jnp.broadcast_to(row, (HALF, HALF)))[:, 0:1].astype(jnp.int32)

    strict = (
        lax.broadcasted_iota(jnp.int32, (HALF, HALF), 1)
        < lax.broadcasted_iota(jnp.int32, (HALF, HALF), 0)
    )
    strict = jnp.where(strict, 1.0, 0.0).astype(bf16)
    expert = lax.broadcasted_iota(jnp.int32, (HALF, EXPERTS), 1)
    slot = lax.broadcasted_iota(jnp.int32, (HALF, SLOTS), 1)
    first, second = column(0), column(1)
    hot0 = jnp.where(expert == first, 1.0, 0.0)
    hot1 = jnp.where(expert == second, 1.0, 0.0)
    before0 = dot(strict, hot0.astype(bf16))
    before1 = dot(strict, hot1.astype(bf16)) + jnp.sum(hot0, axis=0, keepdims=True)
    rank0 = jnp.sum(before0 * hot0, axis=1, keepdims=True).astype(jnp.int32)
    rank1 = jnp.sum(before1 * hot1, axis=1, keepdims=True).astype(jnp.int32)
    return slot == first * 8 + rank0, slot == second * 8 + rank1


def slot_kernel(half, routes, gather):
    hit0, hit1 = slots_of(routes, half)
    gather[...] = jnp.transpose(jnp.where(hit0 | hit1, 1.0, 0.0)).astype(bf16)


def slots(half, routes):
    return pl.pallas_call(
        functools.partial(slot_kernel, half),
        out_shape=jax.ShapeDtypeStruct((SLOTS, HALF), bf16),
        in_specs=[VMEM],
        out_specs=VMEM,
        name="slots",
        compiler_params=ROOM,
    )(routes)


def norm(values, gain, shift):
    mean = jnp.mean(values, axis=-1, keepdims=True)
    center = values - mean
    var = jnp.mean(center * center, axis=-1, keepdims=True)
    return center * lax.rsqrt(var + epsilon) * gain + shift


def mix_kernel(
    half, m0, m1, m2, m3, weight, residual, gain, shift, gather, rows_out, res, rows, sems
):
    tp = lax.axis_index("tp")
    load = pltpu.make_async_copy(residual.at[pl.ds(half * HALF, HALF), :], res, sems.at[CHUNKS])
    load.start()
    branch = None
    for d, m in enumerate((m0, m1, m2, m3)):
        group = (tp + 4 - d) % 4
        row = pl.multiple_of(group * CHANNELS, CHANNELS)
        term = dot(m[...], weight[pl.ds(row, CHANNELS), :])
        branch = term if branch is None else branch + term
    load.wait()
    values = skip_scale * res[...].astype(f32) + branch
    normed = norm(values, gain[...], shift[...]).astype(bf16)
    stores = []
    for c in range(CHUNKS):
        part = slice(c * SLOTS // CHUNKS, (c + 1) * SLOTS // CHUNKS)
        rows[part, :] = dot(gather[part, :], normed).astype(bf16)
        stores.append(pltpu.make_async_copy(rows.at[part, :], rows_out.at[part, :], sems.at[c]))
        stores[-1].start()
    for store in stores:
        store.wait()


def mix(half, parts, weight, residual, gain, shift, gather):
    return pl.pallas_call(
        functools.partial(mix_kernel, half),
        out_shape=jax.ShapeDtypeStruct((SLOTS, WIDTH), bf16),
        in_specs=[VMEM] * 5 + [HBM] + [VMEM] * 3,
        out_specs=HBM,
        scratch_shapes=[
            pltpu.VMEM((HALF, WIDTH), bf16),
            pltpu.VMEM((SLOTS, WIDTH), bf16),
            pltpu.SemaphoreType.DMA((CHUNKS + 1,)),
        ],
        name="mix",
        compiler_params=ROOM,
    )(*parts, weight, in_hbm(residual), gain, shift, gather)


def weight_kernel(half, laid_out, group_router, expert_router, routes, normed, split):
    hit0, hit1 = slots_of(routes, half)
    rows = dot(jnp.where(hit0, 1.0, 0.0).astype(bf16), laid_out[...]).astype(bf16)
    normed[...] = rows
    group_logits = dot(rows, group_router[...])
    expert_logits = dot(rows, expert_router[...])
    group_exp = jnp.exp(group_logits)
    group_prob = group_exp / jnp.sum(group_exp, axis=1, keepdims=True)
    slot = lax.broadcasted_iota(jnp.int32, (EXPERTS, SLOTS), 1)
    expert = lax.broadcasted_iota(jnp.int32, (EXPERTS, SLOTS), 0)
    widen = jnp.where(slot // 8 == expert, 1.0, 0.0)
    slot = lax.broadcasted_iota(jnp.int32, (4, SLOTS), 1)
    group = lax.broadcasted_iota(jnp.int32, (4, SLOTS), 0)
    widen_group = jnp.where(slot // (SLOTS // 4) == group, 1.0, 0.0)
    logits = dot(expert_logits, widen, precision=lax.Precision.HIGHEST)
    share = dot(group_prob, widen_group, precision=lax.Precision.HIGHEST)
    hit = hit0 | hit1
    picked_exp = jnp.where(hit, jnp.exp(logits), 0.0)
    pair_share = picked_exp / jnp.sum(picked_exp, axis=1, keepdims=True)
    weight = jnp.where(hit, share * pair_share, 0.0)
    high = weight.astype(bf16)
    split[0:HALF, :] = high
    split[HALF:, :] = (weight - high.astype(f32)).astype(bf16)


def weights(half, laid_out, group_router, expert_router, routes):
    return pl.pallas_call(
        functools.partial(weight_kernel, half),
        out_shape=[
            jax.ShapeDtypeStruct((HALF, WIDTH), bf16),
            jax.ShapeDtypeStruct((2 * HALF, SLOTS), bf16),
        ],
        in_specs=[VMEM] * 4,
        out_specs=[VMEM] * 2,
        name="weights",
    )(laid_out, group_router, expert_router, routes)


def finish_kernel(split, returned, normed, gain, shift, *rest):
    out = rest[-1]
    both = dot(split[...], returned[...])
    routed = both[0:HALF, :] + both[HALF:, :]
    values = skip_scale * normed[...].astype(f32) + routed
    out[...] = norm(values, gain[...], shift[...]).astype(bf16)


def finish(half, split, returned, normed, gain, shift, base=None):
    def full(*shape):
        return pl.BlockSpec(shape, lambda i: (0,) * len(shape))

    operands = [split, returned, normed, gain, shift]
    in_specs = [full(*a.shape) for a in operands]
    aliases = {}
    if base is not None:
        operands.append(base)
        in_specs.append(HBM)
        aliases = {5: 0}
    return pl.pallas_call(
        finish_kernel,
        grid=(1,),
        out_shape=jax.ShapeDtypeStruct((2 * HALF, WIDTH), bf16),
        in_specs=in_specs,
        out_specs=pl.BlockSpec((HALF, WIDTH), lambda i: (half, 0)),
        input_output_aliases=aliases,
        name="finish",
    )(*operands)


def expert_ffn(arrived, expert_gate, expert_up, expert_down):
    gate_out = jnp.dot(arrived, expert_gate[0], preferred_element_type=f32)
    up_out = jnp.dot(arrived, expert_up[0], preferred_element_type=f32)
    hidden = (jax.nn.silu(gate_out) * up_out).astype(bf16)
    return jnp.dot(hidden, expert_down[0], preferred_element_type=f32).astype(bf16)


def exchange(rows):
    blocks = rows.reshape(EXPERTS, SLOTS // EXPERTS, WIDTH)
    moved = lax.all_to_all(blocks, "sp", split_axis=0, concat_axis=0, tiled=True)
    return moved.reshape(SLOTS, WIDTH)


def on_device(
    residual,
    pool_input,
    doc_ids,
    pool_map,
    pool_scale,
    out_weight,
    mix_gain,
    mix_shift,
    group_router,
    expert_router,
    expert_gate,
    expert_up,
    expert_down,
    routes,
    ffn_gain,
    ffn_shift,
):
    sp_count = lax.axis_size("sp")
    docs = doc_ids.reshape(doc_ids.shape[0] // BLK, BLK)
    inputs = (pool_input, docs, pool_map, pool_scale[None, :])
    flat_routes = routes.T
    parts, tail = {}, None
    for h in (1, 0):
        blocks = pool(h, *inputs, tail=tail, weight=out_weight)
        parts[h] = [blocks[0]] + [
            lax.ppermute(blocks[d], "tp", [(i, (i + d) % 4) for i in range(4)])
            for d in range(1, 4)
        ]
        if h == 1:
            tail = lax.ppermute(blocks[4], "sp", [(i, i + 1) for i in range(sp_count - 1)])
            near_weight = pltpu.with_memory_space_constraint(blocks[5], pltpu.VMEM)
    arrived, kept = {}, {}
    for h in (1, 0):
        gather = slots(h, flat_routes)
        outgoing = mix(
            h,
            parts[h],
            (out_weight, near_weight)[h],
            residual,
            mix_gain[None, :],
            mix_shift[None, :],
            gather,
        )
        arrived[h] = exchange(outgoing)
        kept[h] = weights(h, outgoing, group_router, expert_router, flat_routes)
    result = None
    for h in (1, 0):
        returned = exchange(expert_ffn(arrived[h], expert_gate, expert_up, expert_down))
        normed, split = kept[h]
        result = finish(
            h, split, returned, normed, ffn_gain[None, :], ffn_shift[None, :], result
        )
    return result


def solution(mesh):
    in_specs = (
        P(("sp", "tp"), None),
        P("sp", "tp"),
        P("sp"),
        P("tp", None, None),
        P("tp"),
        P(),
        P(),
        P(),
        P(),
        P(),
        P("sp", None, None),
        P("sp", None, None),
        P("sp", None, None),
        P(("sp", "tp"), None),
        P(),
        P(),
    )
    out_specs = P(("sp", "tp"), None)
    return jax.shard_map(
        on_device, mesh=mesh, in_specs=in_specs, out_specs=out_specs, check_vma=False
    )
```
